768 devices in a mesh: fs: 24 (over z, core), tp: 32 (over y, x).
Axes of the slice: x: 4, y: 8, z: 12, core: 2. Of those that a mesh axis runs over, the one named last changes fastest.
Arguments:
- inputs: bfloat16 [6144, 2016], P('fs'), may hold values from -6 to 6
- pre_act: bfloat16 [6144, 4032], P('fs', 'tp'), may hold values from -6 to 6
- cotangent: bfloat16 [6144, 2016], P('fs'), may hold values from -6 to 6
- w_up: bfloat16 [2016, 4032], P('fs', 'tp'), may hold values from -0.125 to 0.125
- w_down: bfloat16 [4032, 2016], P('tp', 'fs'), may hold values from -0.09375 to 0.09375
Outputs:
- grad_input: bfloat16 [6144, 2016], P('fs')
- grad_up: float32 [2016, 4032], P('fs', 'tp')
- grad_down: float32 [4032, 2016], P('tp', 'fs')
The draws below stay inside these ranges and needn't reach their ends.
All inputs are finite; a program needn't handle non-finite values.
Results may differ from the reference program's by a relative error of at most 0.017.
Values may be sent and summed in bfloat16 or wider, within the bound.
A program may use at most 32 MiB of HBM per device.

```python
import jax
import jax.numpy as jnp
from jax import lax

D = 2016
FF = 4032
TOKENS = 6144
N_TP = 32


def strengthened(entries, rng, source, target, blocks, factor):
    def block_of(position):
        return (jnp.arange(entries.shape[position]) // (entries.shape[position] // blocks)).reshape((-1,) + (1,) * (entries.ndim - 1 - position))

    one_side = jax.random.permutation(rng, blocks)[block_of(target)]
    far = (block_of(target) + blocks // 2) % blocks
    return jnp.where((block_of(source) == one_side) | (block_of(source) == far), factor * entries, entries)


def block_levels(stream_key, shape, split, least, largest):
    def one(axis_at, shards_of):
        steps = jax.random.uniform(jax.random.fold_in(jax.random.fold_in(stream_key, 6), axis_at), (shards_of,), jnp.float32, least / len(split), largest / len(split))
        return jnp.repeat(jnp.exp(steps), shape[axis_at] // shards_of).reshape((-1,) + (1,) * (len(shape) - axis_at - 1))

    factor_of = one(*split[0])
    for cut in split[1:]:
        factor_of = factor_of * one(*cut)
    return factor_of


def gaussian(key, extent, spread, limit, cuts=(), dtype=jnp.bfloat16):
    loudness = block_levels(key, extent, cuts, -0.22, 0.18) if cuts else 1.0
    result = jax.random.normal(key, extent, jnp.float32) * spread * loudness
    return jnp.minimum(jnp.maximum(result, -limit), limit).astype(dtype)


def bell_draw_with(stream_key, shape, deviation, most, split, heavy, held_as=jnp.bfloat16):
    result = deviation * jax.random.normal(stream_key, shape, jnp.float32)
    if split:
        result = result * block_levels(stream_key, shape, split, -0.22, 0.18)
    return jnp.clip(strengthened(result, jax.random.fold_in(stream_key, 3), *heavy), -most, most).astype(held_as)


def setup_inputs(seed: int = 0) -> dict:
    key_of = jax.random.split(jax.random.key(seed), 6)
    inputs = bell_draw_with(key_of[0], (TOKENS, D), 1.0, 6.0, ((0, 24),), (0, 1, 24, 2.25))
    pre_act = gaussian(key_of[1], (TOKENS, FF), 1.0, 6.0, ((0, 24), (1, 32)))
    cotangent = bell_draw_with(key_of[2], (TOKENS, D), 1.0, 6.0, ((0, 24),), (0, 1, 24, 2.25))
    w_up = gaussian(key_of[3], (D, FF), D ** -0.5, 0.125, ((0, 24), (1, 32)))
    w_down = gaussian(key_of[4], (FF, D), FF ** -0.5, 0.09375, ((0, 32), (1, 24)))
    return {"inputs": inputs, "pre_act": pre_act, "cotangent": cotangent, "w_up": w_up, "w_down": w_down}


def reference(inputs, pre_act, cotangent, w_up, w_down):
    positive = jnp.maximum(pre_act.astype(jnp.float32), 0.0)
    hidden = (positive * positive).astype(jnp.bfloat16)
    hidden_grad = lax.dot_general(cotangent, w_down, (((1,), (1,)), ((), ())), preferred_element_type=jnp.float32)
    pre_grad = (2.0 * positive * hidden_grad).astype(jnp.bfloat16)
    grad_down = lax.dot_general(hidden, cotangent, (((0,), (0,)), ((), ())), preferred_element_type=jnp.float32)
    grad_up = lax.dot_general(inputs, pre_grad, (((0,), (0,)), ((), ())), preferred_element_type=jnp.float32)
    width = FF // N_TP

    def add_block(index, total):
        start = (index * width).astype(jnp.int32)
        piece_grad = lax.dynamic_slice_in_dim(pre_grad, start, width, 1)
        piece_weight = lax.dynamic_slice_in_dim(w_up, start, width, 1)
        partial_sum = lax.dot_general(piece_grad, piece_weight, (((1,), (1,)), ((), ())), preferred_element_type=jnp.float32).astype(jnp.bfloat16)
        partial_sum = lax.optimization_barrier(partial_sum)
        return total + partial_sum.astype(jnp.float32)

    total = lax.fori_loop(0, N_TP, add_block, jnp.zeros((TOKENS, D), jnp.float32))
    return total.astype(jnp.bfloat16), grad_up, grad_down
```

```python
import functools

import jax
import jax.numpy as jnp
from jax import lax
from jax.experimental import pallas as pl
from jax.experimental.pallas import tpu as pltpu
from jax.sharding import Mesh
from jax.sharding import PartitionSpec as P

AXES = ("z", "c", "y", "x")
NZ, NC, NY, NX = 12, 2, 8, 4
MESH_IDS = pl.DeviceIdType.MESH
F32 = jnp.float32
BF16 = jnp.bfloat16
TOK, D, WID, BLK = 256, 2016, 126, 84
DP, ROWS = 2048, 96
CHUNKS = 4
CR = TOK // NX // CHUNKS
YL = DP // NY


def kernel(
    inputs_hbm, pre_hbm, cot_hbm, wup_hbm, wdown_hbm,
    gi_out, gup_out, gdown_out,
    inp, pre, cot, wup, wdn,
    scr, pact, wc, grad, wg, pgrad, part, xr, xs, yr, gi,
    gs, sib, cs, zr,
    ld_sem, out_sem, ag_recv, ag_sib, ag_send,
    sib_send, sib_recv, z_send, z_recv,
    x_send, x_recv, y_send, y_recv, ay_send, ay_recv, ax_send, ax_recv,
):
    z, c, y, x = (lax.axis_index(a) for a in AXES)

    def zpeer(d):
        return {"z": lax.rem(z + (d + NZ), NZ)}

    def ypeer(d):
        return {"y": lax.rem(y + d, NY)}

    def xpeer(d):
        return {"x": lax.rem(x + d, NX)}

    other = {"c": 1 - c}

    def send(src, dst, ssem, rsem, to):
        pltpu.make_async_remote_copy(
            src_ref=src, dst_ref=dst, send_sem=ssem, recv_sem=rsem,
            device_id=to, device_id_type=MESH_IDS,
        ).start()

    def wait(ref, sem):
        pltpu.make_async_copy(ref, ref, sem).wait()

    loads = [
        pltpu.make_async_copy(a, b, ld_sem.at[i])
        for i, (a, b) in enumerate(
            ((wdown_hbm, wdn), (wup_hbm, wup), (pre_hbm, pre), (cot_hbm, cot), (inputs_hbm, inp))
        )
    ]
    for copy in loads:
        copy.start()

    barrier = pltpu.get_barrier_semaphore()
    peers = [zpeer(d) for d in range(1, NZ)] + [other]
    peers += [xpeer(d) for d in range(1, NX)] + [ypeer(d) for d in range(1, NY)]
    for to in peers:
        pl.semaphore_signal(barrier, inc=1, device_id=to, device_id_type=MESH_IDS)

    mine = 2 * z + c
    scr[...] = jnp.zeros_like(scr)
    loads[0].wait()
    scr[0:WID, 0:BLK] = wdn[...].astype(F32)
    wg[0, mine] = scr[...].T[0:ROWS].astype(BF16)
    scr[...] = jnp.zeros_like(scr)
    loads[1].wait()
    scr[0:BLK, 0:WID] = wup[...].astype(F32)
    wg[1, mine] = scr[0:ROWS].astype(BF16)

    pl.semaphore_wait(barrier, len(peers))

    def block_from(d):
        return 2 * lax.rem(z - d + NZ, NZ) + c

    def ag_first(w):
        ref = wg.at[w, mine]
        for d in (3, -3, 2, -2, 1, -1):
            send(ref, ref, ag_send.at[w], ag_recv.at[w, d % NZ], zpeer(d))
        send(ref, ref, ag_send.at[w], ag_sib.at[w, 0], other)

    def ag_arrived(w, d):
        ref = wg.at[w, block_from(d)]
        wait(ref, ag_recv.at[w, d % NZ])

    def ag_pass(w, d):
        ref = wg.at[w, block_from(d)]
        send(ref, ref, ag_send.at[w], ag_sib.at[w, d % NZ], other)

    def ag_relay(w):
        for d in (3, -3):
            ag_arrived(w, d)
        far = wg.at[w, 2 * lax.rem(z + (NZ - 3) + 6 * c, NZ) + c]
        send(far, far, ag_send.at[w], ag_recv.at[w, 6], {"z": lax.rem(z + (NZ + 3) - 6 * c, NZ)})
        for step in (2, 1):
            for s in (1, -1):
                ref = wg.at[w, block_from(3 * s)]
                d = s * (3 + step)
                send(ref, ref, ag_send.at[w], ag_recv.at[w, d % NZ], zpeer(s * step))
        for d in (3, -3):
            ag_pass(w, d)

    def ag_near(w):
        for d in (2, -2, 1, -1):
            ag_arrived(w, d)
            ag_pass(w, d)

    def ag_far(w):
        for d in (4, -4, 5, -5, 6):
            ag_arrived(w, d)
            ag_pass(w, d)

    def ag_last(w):
        for d in range(NZ):
            ref = wg.at[w, 2 * lax.rem(z - d + NZ, NZ) + 1 - c]
            wait(ref, ag_sib.at[w, d])

    def compact(w):
        for f in range(2 * NZ):
            wc[f * BLK : f * BLK + ROWS, :] = wg[w, f].astype(F32)

    def to_blocks(g):
        for f in range(2 * NZ):
            gs[g, f % 2, f // 2] = grad[f * BLK : f * BLK + ROWS, :].astype(BF16)

    def pair_send(g):
        send(gs.at[g, 1 - c], sib.at[g], sib_send.at[g], sib_recv.at[g], other)

    def pair_sum(g):
        wait(sib.at[g], sib_recv.at[g])
        for k in range(NZ):
            cs[g, k] = (gs[g, c, k].astype(F32) + sib[g, k].astype(F32)).astype(BF16)

    def z_out(g):
        for d in (6, 5, -5, 4, -4, 3, -3, 2, -2, 1, -1):
            to = lax.rem(z + (d + NZ), NZ)
            send(cs.at[g, to], zr.at[g, d % NZ - 1], z_send.at[g], z_recv.at[g], {"z": to})

    def z_sum(g):
        wait(zr.at[g], z_recv.at[g])
        total = cs[g, z].astype(F32)
        for k in range(NZ - 1):
            total = total + zr[g, k].astype(F32)
        return total

    ag_first(0)
    ag_first(1)

    wc[2016:DP, :] = jnp.zeros((DP - 2016, 128), F32)
    grad[2016:DP, :] = jnp.zeros((DP - 2016, 128), F32)
    pact[...] = jnp.zeros_like(pact)
    loads[2].wait()
    pact[:, 0:WID] = jnp.maximum(pre[...].astype(F32), 0.0)
    positive = pact[...]
    hidden = (positive * positive).astype(BF16)
    ag_relay(0)
    loads[3].wait()
    grad[0:D, :] = lax.dot_general(
        cot[...], hidden, (((0,), (0,)), ((), ())), preferred_element_type=F32
    )
    to_blocks(0)
    pair_send(0)
    ag_near(0)
    ag_relay(1)
    ag_near(1)
    ag_far(0)
    ag_last(0)
    compact(0)
    hidden_grad = jnp.dot(cot[...], wc[0:D, :].astype(BF16), preferred_element_type=F32)
    pgrad[...] = (2.0 * pact[...] * hidden_grad).astype(BF16)
    ag_far(1)
    ag_last(1)
    compact(1)

    def rows_of(share, k):
        return pl.ds(pl.multiple_of(share * (TOK // NX) + k * CR, CR), CR)

    weights = wc[...].astype(BF16)
    part[...] = lax.dot_general(
        pgrad[...], weights, (((1,), (1,)), ((), ())), preferred_element_type=F32
    ).astype(BF16)
    for k in range(CHUNKS):
        for d in (2, 1, 3):
            to = lax.rem(x + d, NX)
            send(part.at[rows_of(to, k), :], xr.at[k, d - 1], x_send.at[k], x_recv.at[k], {"x": to})

    pair_sum(0)
    z_out(0)
    loads[4].wait()
    grad[0:D, :] = lax.dot_general(
        inp[...], pgrad[...], (((0,), (0,)), ((), ())), preferred_element_type=F32
    )
    to_blocks(1)
    pair_send(1)

    def own_lanes(who):
        return pl.ds(pl.multiple_of(who * YL, YL), YL)

    def x_step(k):
        wait(xr.at[k], x_recv.at[k])
        total = part[rows_of(x, k), :].astype(F32)
        for j in range(NX - 1):
            total = total + xr[k, j].astype(F32)
        xs[k] = total.astype(BF16)
        for d in (4, 3, 5, 2, 6, 1, 7):
            to = lax.rem(y + d, NY)
            send(xs.at[k, :, own_lanes(to)], yr.at[k, d - 1], y_send.at[k], y_recv.at[k], {"y": to})

    def y_step(k):
        wait(yr.at[k], y_recv.at[k])
        total = xs[k, :, own_lanes(y)].astype(F32)
        for j in range(NY - 1):
            total = total + yr[k, j].astype(F32)
        gi[rows_of(x, k), own_lanes(y)] = total.astype(BF16)
        ref = gi.at[rows_of(x, k), own_lanes(y)]
        for d in (4, 3, 5, 2, 6, 1, 7):
            send(ref, ref, ay_send.at[k], ay_recv.at[k], ypeer(d))

    def ay_step(k):
        wait(yr.at[k], ay_recv.at[k])
        ref = gi.at[rows_of(x, k), :]
        for d in (2, 1, 3):
            send(ref, ref, ax_send.at[k], ax_recv.at[k], xpeer(d))

    def ax_step(k):
        wait(xr.at[k], ax_recv.at[k])
        for s in range(NX):
            rows = slice(s * (TOK // NX) + k * CR, s * (TOK // NX) + (k + 1) * CR)
            pltpu.make_async_copy(gi.at[rows, :], gi_out.at[rows, :], out_sem.at[k, s]).start()

    x_step(0)
    x_step(1)
    pair_sum(1)
    z_out(1)
    y_step(0)
    x_step(2)
    y_step(1)
    x_step(3)
    ay_step(0)
    y_step(2)
    ay_step(1)
    y_step(3)
    ay_step(2)
    ax_step(0)
    ay_step(3)
    ax_step(1)
    down = z_sum(0)
    scr[...] = jnp.zeros_like(scr)
    scr[0:ROWS, :] = down
    gdown_out[...] = scr[...].T[0:WID, 0:BLK]
    ax_step(2)
    gup_out[...] = z_sum(1)[0:BLK, 0:WID]
    ax_step(3)

    for w in range(2):
        wait(wg.at[w, pl.ds(0, 23)], ag_send.at[w])
        wait(sib.at[w], sib_send.at[w])
        wait(zr.at[w], z_send.at[w])
    for k in range(CHUNKS):
        wait(xr.at[k], x_send.at[k])
        wait(yr.at[k], y_send.at[k])
        wait(yr.at[k], ay_send.at[k])
        wait(xr.at[k], ax_send.at[k])
        for s in range(NX):
            rows = slice(s * (TOK // NX) + k * CR, s * (TOK // NX) + (k + 1) * CR)
            pltpu.make_async_copy(gi.at[rows, :], gi_out.at[rows, :], out_sem.at[k, s]).wait()


def on_device(inputs, pre_act, cotangent, w_up, w_down):
    any_space = pl.BlockSpec(memory_space=pl.ANY)
    in_vmem = pl.BlockSpec(memory_space=pltpu.VMEM)
    dma = pltpu.SemaphoreType.DMA
    grad_input, grad_up, grad_down = pl.pallas_call(
        kernel,
        out_shape=(
            jax.ShapeDtypeStruct((TOK, DP), BF16),
            jax.ShapeDtypeStruct((BLK, WID), F32),
            jax.ShapeDtypeStruct((WID, BLK), F32),
        ),
        in_specs=[any_space] * 5,
        out_specs=(any_space, in_vmem, in_vmem),
        scratch_shapes=[
            pltpu.VMEM((TOK, D), BF16),
            pltpu.VMEM((TOK, WID), BF16),
            pltpu.VMEM((TOK, D), BF16),
            pltpu.VMEM((BLK, WID), BF16),
            pltpu.VMEM((WID, BLK), BF16),
            pltpu.VMEM((128, 128), F32),
            pltpu.VMEM((TOK, 128), F32),
            pltpu.VMEM((DP, 128), F32),
            pltpu.VMEM((DP, 128), F32),
            pltpu.VMEM((2, 2 * NZ, ROWS, 128), BF16),
            pltpu.VMEM((TOK, 128), BF16),
            pltpu.VMEM((TOK, DP), BF16),
            pltpu.VMEM((CHUNKS, NX - 1, CR, DP), BF16),
            pltpu.VMEM((CHUNKS, CR, DP), BF16),
            pltpu.VMEM((CHUNKS, NY - 1, CR, YL), BF16),
            pltpu.VMEM((TOK, DP), BF16),
            pltpu.VMEM((2, 2, NZ, ROWS, 128), BF16),
            pltpu.VMEM((2, NZ, ROWS, 128), BF16),
            pltpu.VMEM((2, NZ, ROWS, 128), BF16),
            pltpu.VMEM((2, NZ - 1, ROWS, 128), BF16),
            dma((5,)), dma((CHUNKS, NX)), dma((2, NZ)), dma((2, NZ)), dma((2,)),
            dma((2,)), dma((2,)), dma((2,)), dma((2,)),
            dma((CHUNKS,)), dma((CHUNKS,)), dma((CHUNKS,)), dma((CHUNKS,)),
            dma((CHUNKS,)), dma((CHUNKS,)), dma((CHUNKS,)), dma((CHUNKS,)),
        ],
        compiler_params=pltpu.CompilerParams(
            collective_id=0, has_side_effects=True, vmem_limit_bytes=48 << 20
        ),
    )(inputs, pre_act, cotangent, w_up, w_down)
    return grad_input[:, :D], grad_up, grad_down


def solution(mesh):
    split = Mesh(mesh.devices.reshape(NZ, NC, NY, NX), AXES)
    fs, tp = ("z", "c"), ("y", "x")
    return jax.shard_map(
        on_device,
        mesh=split,
        in_specs=(P(fs, None), P(fs, tp), P(fs, None), P(fs, tp), P(tp, fs)),
        out_specs=(P(fs, None), P(fs, tp), P(tp, fs)),
        check_vma=False,
    )
```

```python
import functools

import jax
import jax.numpy as jnp
from jax import lax
from jax.experimental import pallas as pl
from jax.experimental.pallas import tpu as pltpu
from jax.sharding import Mesh
from jax.sharding import PartitionSpec as P

AXES = ("z", "c", "y", "x")
NZ, NC, NY, NX = 12, 2, 8, 4
MESH_IDS = pl.DeviceIdType.MESH
F32 = jnp.float32
BF16 = jnp.bfloat16
TOK, D, WID, BLK = 256, 2016, 126, 84
DP, ROWS = 2048, 96
LANES, QUARTERS, RB = 128, 4, 16
CHUNKS = [(h, q) for h in range(TOK // LANES) for q in range(QUARTERS)]
Y_FIRST = (1,)
X_FIRST = tuple(i for i in range(len(CHUNKS)) if i not in Y_FIRST)
ORDER = tuple(range(len(CHUNKS)))
X_TIMES = (3.8, 8.4, 13.0)
Y_TIMES = (7.5, 11.0, 14.5)
X_STEP, Y_STEP = 1.4, 3.0


def kernel(
    inputs_hbm, pre_hbm, cot_hbm, wup_hbm, wdown_hbm,
    gi, gup_out, gdown_out,
    inp, pre, cot, wup, wdn,
    cotn, scr, pact, wc, grad, wg, pgrad, pgt, part,
    x_in1, x_sum, y_in2, y_in1, y_sum, x_in2,
    gs, sib, cs, zr,
    ld_sem, ag_recv, ag_sib, ag_send,
    sib_send, sib_recv, z_send, z_recv,
    s1, r1, s2, r2, s3, r3, s4, r4,
):
    z, c, y, x = (lax.axis_index(a) for a in AXES)

    def zpeer(d):
        return {"z": lax.rem(z + (d + NZ), NZ)}

    def ypeer(d):
        return {"y": lax.rem(y + d, NY)}

    def xpeer(d):
        return {"x": lax.rem(x + d, NX)}

    other = {"c": 1 - c}

    def send(src, dst, ssem, rsem, to):
        pltpu.make_async_remote_copy(
            src_ref=src, dst_ref=dst, send_sem=ssem, recv_sem=rsem,
            device_id=to, device_id_type=MESH_IDS,
        ).start()

    def wait(ref, sem):
        pltpu.make_async_copy(ref, ref, sem).wait()

    loads = [
        pltpu.make_async_copy(a, b, ld_sem.at[i])
        for i, (a, b) in enumerate(
            ((wdown_hbm, wdn), (wup_hbm, wup), (pre_hbm, pre), (cot_hbm, cot), (inputs_hbm, inp))
        )
    ]
    for copy in loads:
        copy.start()

    barrier = pltpu.get_barrier_semaphore()
    peers = [zpeer(d) for d in (2, -2, 1, -1)] + [other]
    peers += [xpeer(d) for d in range(1, NX)] + [ypeer(d) for d in range(1, NY)]
    for to in peers:
        pl.semaphore_signal(barrier, inc=1, device_id=to, device_id_type=MESH_IDS)

    mine = 2 * z + c
    scr[...] = jnp.zeros_like(scr)
    loads[0].wait()
    scr[0:BLK, 0:WID] = wdn[...].astype(F32)
    wg[0, mine] = scr[...].astype(BF16)
    loads[1].wait()
    scr[0:BLK, 0:WID] = wup[...].astype(F32)
    wg[1, mine] = scr[...].astype(BF16)

    pl.semaphore_wait(barrier, len(peers))

    def block_from(d):
        return 2 * lax.rem(z - d + NZ, NZ) + c

    def ag_own(w, *steps):
        ref = wg.at[w, mine]
        for d in steps:
            send(ref, ref, ag_send.at[w], ag_recv.at[w, d % NZ], zpeer(d))

    def ag_own_pair(w):
        ref = wg.at[w, mine]
        send(ref, ref, ag_send.at[w], ag_sib.at[w, 0], other)

    def ag_wait(w, *ds):
        for d in ds:
            wait(wg.at[w, block_from(d)], ag_recv.at[w, d % NZ])

    def ag_relay(w, d, *steps):
        ref = wg.at[w, block_from(d)]
        for step in steps:
            send(ref, ref, ag_send.at[w], ag_recv.at[w, (d + step) % NZ], zpeer(step))

    def ag_far(w, d):
        @pl.when(c == (0 if d > 0 else 1))
        def _():
            ref = wg.at[w, block_from(d)]
            step = 2 if d > 0 else -2
            send(ref, ref, ag_send.at[w], ag_recv.at[w, 6], zpeer(step))

    def ag_pass(w, *ds):
        for d in ds:
            ref = wg.at[w, block_from(d)]
            send(ref, ref, ag_send.at[w], ag_sib.at[w, d % NZ], other)

    def ag_last(w):
        for d in range(NZ):
            ref = wg.at[w, 2 * lax.rem(z - d + NZ, NZ) + 1 - c]
            wait(ref, ag_sib.at[w, d])

    def compact(w):
        for f in range(2 * NZ):
            wc[f * BLK : f * BLK + ROWS, :] = wg[w, f].astype(F32)

    def to_blocks(g):
        for f in range(2 * NZ):
            gs[g, f % 2, f // 2] = grad[f * BLK : f * BLK + ROWS, :].astype(BF16)

    def pair_send(g):
        send(gs.at[g, 1 - c], sib.at[g], sib_send.at[g], sib_recv.at[g], other)

    def pair_sum(g):
        wait(sib.at[g], sib_recv.at[g])
        for k in range(NZ):
            cs[g, k] = (gs[g, c, k].astype(F32) + sib[g, k].astype(F32)).astype(BF16)

    def z_out(g):
        for d in (6, 5, -5, 4, -4, 3, -3, 2, -2, 1, -1):
            to = lax.rem(z + (d + NZ), NZ)
            send(cs.at[g, to], zr.at[g, d % NZ - 1], z_send.at[g], z_recv.at[g], {"z": to})

    def z_sum(g):
        wait(zr.at[g], z_recv.at[g])
        total = cs[g, z].astype(F32)
        for k in range(NZ - 1):
            total = total + zr[g, k].astype(F32)
        return total

    for w in range(2):
        ag_own(w, 2, -2)
    for w in range(2):
        ag_own_pair(w)

    wc[D:DP, :] = jnp.zeros((DP - D, 128), F32)
    grad[D:DP, :] = jnp.zeros((DP - D, 128), F32)
    pact[...] = jnp.zeros_like(pact)
    loads[2].wait()
    pact[:, 0:WID] = jnp.maximum(pre[...].astype(F32), 0.0)
    positive = pact[...]
    hidden = (positive * positive).astype(BF16)
    loads[3].wait()
    cotn[...] = cot[...].T
    grad[0:D, :] = jnp.dot(cot[...], hidden, preferred_element_type=F32)
    to_blocks(0)
    pair_send(0)

    for w in range(2):
        for d in (2, -2):
            ag_wait(w, d)
            ag_relay(w, d, d)
    for w in range(2):
        ag_own(w, 1, -1)
        ag_pass(w, 2, -2)
    pair_sum(0)
    for w in range(2):
        for d in (4, -4):
            ag_wait(w, d)
            ag_far(w, d)
            ag_relay(w, d, d // 4)
    for w in range(2):
        for d in (2, -2):
            ag_relay(w, d, d // 2)
        ag_pass(w, 4, -4)
    for w in range(2):
        for d in (1, -1):
            ag_wait(w, d)
            ag_pass(w, d)
    for w in range(2):
        for d in (6, 5, -5, 3, -3):
            ag_wait(w, d)
            ag_pass(w, d)
    z_out(0)
    ag_last(0)
    compact(0)
    hidden_grad = jnp.dot(cotn[...], wc[0:D, :].astype(BF16), preferred_element_type=F32)
    pre_grad = 2.0 * pact[...] * hidden_grad
    pgrad[...] = pre_grad.astype(BF16)
    pgt[...] = pre_grad.T.astype(BF16)
    ag_last(1)
    compact(1)

    def others(n):
        return sorted(range(1, n), key=lambda d: -min(d, n - d))

    def scatter(n, me, axis, src, dst, ssem, rsem):
        for d in others(n):
            to = lax.rem(me + d, n)
            send(src(to), dst.at[d - 1], ssem, rsem, {axis: to})

    def share(n, me, axis, ref, ssem, rsem):
        for d in others(n):
            send(ref, ref, ssem, rsem, {axis: lax.rem(me + d, n)})

    def total(own, arrived):
        out = own.astype(F32)
        for j in range(arrived.shape[0]):
            out = out + arrived[j].astype(F32)
        return out.astype(BF16)

    def stage0(i):
        h, q = CHUNKS[i]
        for s in range(NX):
            start = (s * QUARTERS + q) * NY * RB
            rows = wc[start : start + NY * RB, :].astype(BF16)
            half = pgt[:, h * LANES : (h + 1) * LANES]
            product = jnp.dot(rows, half, preferred_element_type=F32).astype(BF16)
            part[h, s, q] = product.reshape(NY, RB, LANES)
        if i in Y_FIRST:
            dst = y_in1.at[Y_FIRST.index(i)]
            scatter(NY, y, "y", lambda to: part.at[h, :, q, to], dst, s1.at[i], r1.at[i])
        else:
            dst = x_in1.at[X_FIRST.index(i)]
            scatter(NX, x, "x", lambda to: part.at[h, to, q], dst, s1.at[i], r1.at[i])

    def stage1(i):
        h, q = CHUNKS[i]
        if i in Y_FIRST:
            j = Y_FIRST.index(i)
            wait(y_in1.at[j], r1.at[i])
            y_sum[j] = total(part[h, :, q, y], y_in1.at[j])
            scatter(NX, x, "x", lambda to: y_sum.at[j, to], x_in2.at[j], s2.at[i], r2.at[i])
        else:
            j = X_FIRST.index(i)
            wait(x_in1.at[j], r1.at[i])
            x_sum[j] = total(part[h, x, q], x_in1.at[j])
            scatter(NY, y, "y", lambda to: x_sum.at[j, to], y_in2.at[j], s2.at[i], r2.at[i])

    def stage2(i):
        h, q = CHUNKS[i]
        ref = gi.at[h, x, q, y]
        if i in Y_FIRST:
            j = Y_FIRST.index(i)
            wait(x_in2.at[j], r2.at[i])
            gi[h, x, q, y] = total(y_sum[j, x], x_in2.at[j])
            share(NX, x, "x", ref, s3.at[i], r3.at[i])
        else:
            j = X_FIRST.index(i)
            wait(y_in2.at[j], r2.at[i])
            gi[h, x, q, y] = total(x_sum[j, y], y_in2.at[j])
            share(NY, y, "y", ref, s3.at[i], r3.at[i])

    def stage3(i):
        h, q = CHUNKS[i]
        if i in Y_FIRST:
            wait(x_in2.at[Y_FIRST.index(i)], r3.at[i])
            share(NY, y, "y", gi.at[h, :, q, y], s4.at[i], r4.at[i])
        else:
            wait(y_in2.at[X_FIRST.index(i)], r3.at[i])
            share(NX, x, "x", gi.at[h, x, q], s4.at[i], r4.at[i])

    def finish(i):
        if i in Y_FIRST:
            j = Y_FIRST.index(i)
            first, second = y_in1.at[j], x_in2.at[j]
        else:
            j = X_FIRST.index(i)
            first, second = x_in1.at[j], y_in2.at[j]
        wait(first, r4.at[i])
        wait(first, s1.at[i])
        wait(second, s2.at[i])
        wait(second, s3.at[i])
        wait(first, s4.at[i])

    for i in ORDER:
        stage0(i)

    loads[4].wait()
    grad[0:D, :] = jnp.dot(inp[...], pgrad[...], preferred_element_type=F32)
    to_blocks(1)
    pair_send(1)

    events = []
    for group, times, step in ((X_FIRST, X_TIMES, X_STEP), (Y_FIRST, Y_TIMES, Y_STEP)):
        for n, stage in enumerate((stage1, stage2, stage3)):
            events += [(times[n] + step * j, i, stage) for j, i in enumerate(group)]
    events.sort(key=lambda e: e[:2])
    for t, (_, i, stage) in enumerate(events):
        stage(i)
        if t == 0:
            pair_sum(1)
            z_out(1)
    gdown_out[...] = z_sum(0)[0:BLK, 0:WID]
    gup_out[...] = z_sum(1)[0:BLK, 0:WID]
    for w in range(2):
        wait(wg.at[w, pl.ds(0, 23)], ag_send.at[w])
        wait(sib.at[w], sib_send.at[w])
        wait(zr.at[w], z_send.at[w])
    for i in ORDER:
        finish(i)


def store(gi, gup, gdown, gi_out, gup_out, gdown_out, sem):
    pairs = [
        (gi.at[h, pl.ds(0, D)], gi_out.at[:, pl.ds(h * LANES, LANES)])
        for h in range(TOK // LANES)
    ]
    pairs += [(gup, gup_out), (gdown, gdown_out)]
    copies = [pltpu.make_async_copy(a, b, sem.at[i]) for i, (a, b) in enumerate(pairs)]
    for copy in copies:
        copy.start()
    for copy in copies:
        copy.wait()


def on_device(inputs, pre_act, cotangent, w_up, w_down):
    in_hbm = pl.BlockSpec(memory_space=pltpu.HBM)
    in_vmem = pl.BlockSpec(memory_space=pltpu.VMEM)
    dma = pltpu.SemaphoreType.DMA
    operands = [
        pltpu.with_memory_space_constraint(a, pltpu.HBM)
        for a in (inputs.T, pre_act, cotangent.T, w_up, w_down.T)
    ]
    grad_input, grad_up, grad_down = pl.pallas_call(
        kernel,
        out_shape=(
            jax.ShapeDtypeStruct((TOK // LANES, NX, QUARTERS, NY, RB, LANES), BF16),
            jax.ShapeDtypeStruct((BLK, WID), F32),
            jax.ShapeDtypeStruct((BLK, WID), F32),
        ),
        in_specs=[in_hbm] * 5,
        out_specs=(in_vmem, in_vmem, in_vmem),
        scratch_shapes=[
            pltpu.VMEM((D, TOK), BF16),
            pltpu.VMEM((TOK, WID), BF16),
            pltpu.VMEM((D, TOK), BF16),
            pltpu.VMEM((BLK, WID), BF16),
            pltpu.VMEM((BLK, WID), BF16),
            pltpu.VMEM((TOK, D), BF16),
            pltpu.VMEM((ROWS, 128), F32),
            pltpu.VMEM((TOK, 128), F32),
            pltpu.VMEM((DP, 128), F32),
            pltpu.VMEM((DP, 128), F32),
            pltpu.VMEM((2, 2 * NZ, ROWS, 128), BF16),
            pltpu.VMEM((TOK, 128), BF16),
            pltpu.VMEM((128, TOK), BF16),
            pltpu.VMEM((TOK // LANES, NX, QUARTERS, NY, RB, LANES), BF16),
            pltpu.VMEM((len(X_FIRST), NX - 1, NY, RB, LANES), BF16),
            pltpu.VMEM((len(X_FIRST), NY, RB, LANES), BF16),
            pltpu.VMEM((len(X_FIRST), NY - 1, RB, LANES), BF16),
            pltpu.VMEM((len(Y_FIRST), NY - 1, NX, RB, LANES), BF16),
            pltpu.VMEM((len(Y_FIRST), NX, RB, LANES), BF16),
            pltpu.VMEM((len(Y_FIRST), NX - 1, RB, LANES), BF16),
            pltpu.VMEM((2, 2, NZ, ROWS, 128), BF16),
            pltpu.VMEM((2, NZ, ROWS, 128), BF16),
            pltpu.VMEM((2, NZ, ROWS, 128), BF16),
            pltpu.VMEM((2, NZ - 1, ROWS, 128), BF16),
            dma((5,)), dma((2, NZ)), dma((2, NZ)), dma((2,)),
            dma((2,)), dma((2,)), dma((2,)), dma((2,)),
            *[dma((len(CHUNKS),)) for _ in range(8)],
        ],
        compiler_params=pltpu.CompilerParams(
            collective_id=0, has_side_effects=True, vmem_limit_bytes=40 << 20
        ),
    )(*operands)
    grad_input, grad_up, grad_down = pl.pallas_call(
        store,
        out_shape=(
            jax.ShapeDtypeStruct((D, TOK), BF16),
            jax.ShapeDtypeStruct((BLK, WID), F32),
            jax.ShapeDtypeStruct((BLK, WID), F32),
        ),
        in_specs=[pl.BlockSpec(memory_space=pl.ANY)] * 3,
        out_specs=(in_hbm,) * 3,
        scratch_shapes=[dma((TOK // LANES + 2,))],
        compiler_params=pltpu.CompilerParams(vmem_limit_bytes=4 << 20),
    )(grad_input.reshape(TOK // LANES, DP, LANES), grad_up, grad_down)
    return grad_input.T, grad_up, grad_down.T


def solution(mesh):
    split = Mesh(mesh.devices.reshape(NZ, NC, NY, NX), AXES)
    fs, tp = ("z", "c"), ("y", "x")
    return jax.shard_map(
        on_device,
        mesh=split,
        in_specs=(P(fs, None), P(fs, tp), P(fs, None), P(fs, tp), P(tp, fs)),
        out_specs=(P(fs, None), P(fs, tp), P(tp, fs)),
        check_vma=False,
    )
```

```python
import functools

import jax
import jax.numpy as jnp
from jax import lax
from jax.experimental import pallas as pl
from jax.experimental.pallas import tpu as pltpu
from jax.sharding import Mesh
from jax.sharding import PartitionSpec as P

AXES = ("z", "c", "y", "x")
NZ, NC, NY, NX = 12, 2, 8, 4
MESH_IDS = pl.DeviceIdType.MESH
F32 = jnp.float32
BF16 = jnp.bfloat16
TOK, D, WID, BLK = 256, 2016, 126, 84
DP, TILES = 2048, 11
ROWS = 8 * TILES
LANES, QUARTERS, RB = 128, 4, 16
CHUNKS = [(h, q) for h in range(TOK // LANES) for q in range(QUARTERS)]
Y_FIRST = (1,)
X_FIRST = tuple(i for i in range(len(CHUNKS)) if i not in Y_FIRST)
ORDER = tuple(range(len(CHUNKS)))
PER_CHUNK = 2 * (NY - 1 + (NX - 1) * NY) * RB // 8
assert PER_CHUNK == 2 * (NX - 1 + (NY - 1) * NX) * RB // 8
SENT = 2 * TILES * (23 + NZ + NZ - 1) + len(CHUNKS) * PER_CHUNK
X_TIMES = (4.3, 9.0, 13.7)
Y_TIMES = (8.5, 15.0, 18.5)
X_STEP, Y_STEP = 1.4, 3.0


def kernel(
    inputs_hbm, pre_hbm, cot_hbm, wup_hbm, wdown_hbm,
    gi, gup_out, gdown_out,
    inp, pre, cot, wup, wdn,
    cotn, scr, pact, wc, grad, wg, pgrad, pgt, part,
    x_in1, x_sum, y_in2, y_in1, y_sum, x_in2, done, gsum,
    gs, sib, cs, zr,
    sent, ld_sem, ag_recv, ag_sib, sib_recv, z_recv,
    r1, r2, r3, r4, met, own_sem, send_sem,
):
    z, c, y, x = (lax.axis_index(a) for a in AXES)

    def zpeer(d):
        return {"z": lax.rem(z + (d + NZ), NZ)}

    def ypeer(d):
        return {"y": lax.rem(y + d, NY)}

    def xpeer(d):
        return {"x": lax.rem(x + d, NX)}

    other = {"c": 1 - c}

    def send(src, dst, rsem, to):
        pltpu.make_async_remote_copy(
            src_ref=src, dst_ref=dst, send_sem=send_sem, recv_sem=rsem,
            device_id=to, device_id_type=MESH_IDS,
        ).start()

    def wait(ref, sem):
        pltpu.make_async_copy(ref, ref, sem).wait()

    loads = [
        pltpu.make_async_copy(a, b, ld_sem.at[i])
        for i, (a, b) in enumerate(
            ((wdown_hbm, wdn), (wup_hbm, wup), (pre_hbm, pre), (cot_hbm, cot), (inputs_hbm, inp))
        )
    ]
    for copy in loads:
        copy.start()

    barrier = pltpu.get_barrier_semaphore()
    peers = [zpeer(d) for d in (3, -3, 2, -2, 1, -1)] + [other]
    peers += [xpeer(1), xpeer(NX - 1), ypeer(1), ypeer(NY - 1)]
    for to in peers:
        pl.semaphore_signal(barrier, inc=1, device_id=to, device_id_type=MESH_IDS)

    mine = 2 * z + c

    def tiles(block):
        return block.reshape(TILES, 8, 128).astype(BF16)

    scr[...] = jnp.zeros_like(scr)
    loads[0].wait()
    scr[0:BLK, 0:WID] = wdn[...].astype(F32)
    wg[0, mine] = tiles(scr[...])
    loads[1].wait()
    scr[0:BLK, 0:WID] = wup[...].astype(F32)
    wg[1, mine] = tiles(scr[...])

    pl.semaphore_wait(barrier, len(peers))

    def meet(r):
        links = [(met.at[r], ypeer(1)), (met.at[3 + r], ypeer(NY - 1))]
        if r == 0:
            links += [(met.at[6], xpeer(1)), (met.at[7], xpeer(NX - 1))]
        for sem, to in links:
            pl.semaphore_signal(sem, inc=1, device_id=to, device_id_type=MESH_IDS)

    def met_all(r):
        for i in (r, 3 + r, *((6, 7) if r == 0 else ())):
            pl.semaphore_wait(met.at[i], 1)

    meet(0)

    near = jnp.where(lax.rem(z + 3, NZ) < NZ // 2, -1, 1)
    sides = (near, -near)

    def slot(d):
        return lax.rem(d + NZ, NZ)

    def block_from(d):
        return 2 * lax.rem(z - d + NZ, NZ) + c

    def ag_own(w, *steps):
        ref = wg.at[w, mine]
        for d in steps:
            send(ref, ref, ag_recv.at[w, d % NZ], zpeer(d))

    def ag_own_pair(w):
        ref = wg.at[w, mine]
        send(ref, ref, ag_sib.at[w], other)

    def ag_wait(w, d):
        wait(wg.at[w, block_from(d)], ag_recv.at[w, slot(d)])

    def ag_relay(w, side):
        ref = wg.at[w, block_from(3 * side)]

        @pl.when(c == (1 - side) // 2)
        def _():
            send(ref, ref, ag_recv.at[w, 6], zpeer(3 * side))

        ag_step(w, 3 * side, side)

        ag_step(w, 3 * side, 2 * side)

    def ag_step(w, d, step):
        ref = wg.at[w, block_from(d)]
        send(ref, ref, ag_recv.at[w, slot(d + step)], zpeer(step))

    def ag_pass(w, d):
        ref = wg.at[w, block_from(d)]
        send(ref, ref, ag_sib.at[w], other)

    def ag_last(w):
        wait(wg.at[w, pl.ds(0, NZ)], ag_sib.at[w])

    def compact(w):
        for f in range(2 * NZ):
            wc[f * BLK : f * BLK + ROWS, :] = wg[w, f].astype(F32).reshape(ROWS, 128)

    def to_blocks(g):
        for f in range(2 * NZ):
            gs[g, f % 2, f // 2] = tiles(grad[f * BLK : f * BLK + ROWS, :])

    def pair_send(g):
        send(gs.at[g, 1 - c], sib.at[g], sib_recv.at[g], other)

    def pair_sum(g):
        wait(sib.at[g], sib_recv.at[g])
        for k in range(NZ):
            cs[g, k] = (gs[g, c, k].astype(F32) + sib[g, k].astype(F32)).astype(BF16)

    def z_out(g):
        for d in (6, 5, -5, 4, -4, 3, -3, 2, -2, 1, -1):
            to = lax.rem(z + (d + NZ), NZ)
            send(cs.at[g, to], zr.at[g, d % NZ - 1], z_recv.at[g], {"z": to})

    def z_sum(g):
        wait(zr.at[g], z_recv.at[g])
        total = cs[g, z].astype(F32)
        for k in range(NZ - 1):
            total = total + zr[g, k].astype(F32)
        return total

    for w in range(2):
        ag_own(w, 3, -3)
    for w in range(2):
        ag_own_pair(w)
        ag_own(w, 1, -1)

    wc[D:DP, :] = jnp.zeros((DP - D, 128), F32)
    grad[D:DP, :] = jnp.zeros((DP - D, 128), F32)
    pact[...] = jnp.zeros_like(pact)
    loads[2].wait()
    pact[:, 0:WID] = jnp.maximum(pre[...].astype(F32), 0.0)
    positive = pact[...]
    hidden = (positive * positive).astype(BF16)
    loads[3].wait()
    cotn[...] = cot[...].T
    grad[0:D, :] = jnp.dot(cot[...], hidden, preferred_element_type=F32)
    to_blocks(0)
    pair_send(0)

    for w in range(2):
        for side in sides:
            ag_wait(w, 3 * side)
            ag_relay(w, side)
    met_all(0)
    meet(1)
    for w in range(2):
        for side in sides:
            ag_wait(w, side)
            ag_step(w, side, side)
    for w in range(2):
        for side in sides:
            ag_pass(w, 3 * side)
            ag_pass(w, side)
    for w in range(2):
        for side in sides:
            ag_wait(w, 4 * side)
    pair_sum(0)
    met_all(1)
    meet(2)

    def ag_end(w):
        for side in sides:
            ag_pass(w, 4 * side)
        for side in sides:
            ag_wait(w, 2 * side)
            ag_pass(w, 2 * side)
        ag_wait(w, 6)
        ag_pass(w, 6)
        for side in sides:
            ag_wait(w, 5 * side)
            ag_pass(w, 5 * side)

    ag_end(0)
    ag_end(1)
    ag_last(0)
    compact(0)
    hidden_grad = jnp.dot(cotn[...], wc[0:D, :].astype(BF16), preferred_element_type=F32)
    pre_grad = 2.0 * pact[...] * hidden_grad
    pgrad[...] = pre_grad.astype(BF16)
    pgt[...] = pre_grad.T.astype(BF16)
    met_all(2)
    ag_last(1)
    compact(1)

    def others(n):
        return sorted(range(1, n), key=lambda d: -min(d, n - d))

    def scatter(n, me, axis, src, dst, rsem):
        for d in others(n):
            to = lax.rem(me + d, n)
            send(src(to), dst.at[d - 1], rsem, {axis: to})

    def share(n, me, axis, src, dst, rsem):
        for d in others(n):
            send(src, dst, rsem, {axis: lax.rem(me + d, n)})

    def total(own, arrived):
        out = own.astype(F32)
        for j in range(arrived.shape[0]):
            out = out + arrived[j].astype(F32)
        return out.astype(BF16)

    def stage0(i):
        h, q = CHUNKS[i]
        for s in range(NX):
            start = (s * QUARTERS + q) * NY * RB
            rows = wc[start : start + NY * RB, :].astype(BF16)
            half = pgt[:, h * LANES : (h + 1) * LANES]
            product = jnp.dot(rows, half, preferred_element_type=F32).astype(BF16)
            part[h, s, q] = product.reshape(NY, RB, LANES)
        if i in Y_FIRST:
            dst = y_in1.at[Y_FIRST.index(i)]
            scatter(NY, y, "y", lambda to: part.at[h, :, q, to], dst, r1.at[i])
        else:
            dst = x_in1.at[X_FIRST.index(i)]
            scatter(NX, x, "x", lambda to: part.at[h, to, q], dst, r1.at[i])

    def stage1(i):
        h, q = CHUNKS[i]
        if i in Y_FIRST:
            j = Y_FIRST.index(i)
            wait(y_in1.at[j], r1.at[i])
            y_sum[j] = total(part[h, :, q, y], y_in1.at[j])
            scatter(NX, x, "x", lambda to: y_sum.at[j, to], x_in2.at[j], r2.at[i])
        else:
            j = X_FIRST.index(i)
            wait(x_in1.at[j], r1.at[i])
            x_sum[j] = total(part[h, x, q], x_in1.at[j])
            scatter(NY, y, "y", lambda to: x_sum.at[j, to], y_in2.at[j], r2.at[i])

    def stage2(i):
        h, q = CHUNKS[i]
        to = gi.at[h, x, q, y]
        if i in Y_FIRST:
            j = Y_FIRST.index(i)
            wait(x_in2.at[j], r2.at[i])
            done[i] = total(y_sum[j, x], x_in2.at[j])
            share(NX, x, "x", done.at[i], to, r3.at[i])
        else:
            j = X_FIRST.index(i)
            wait(y_in2.at[j], r2.at[i])
            done[i] = total(x_sum[j, y], y_in2.at[j])
            share(NY, y, "y", done.at[i], to, r3.at[i])
        pltpu.make_async_copy(done.at[i], to, own_sem.at[i]).start()

    def stage3(i):
        h, q = CHUNKS[i]
        pltpu.make_async_copy(done.at[i], gi.at[h, x, q, y], own_sem.at[i]).wait()
        if i in Y_FIRST:
            wait(x_in2.at[Y_FIRST.index(i)], r3.at[i])
            part_of_all = gi.at[h, :, q, y]
            share(NY, y, "y", part_of_all, part_of_all, r4.at[i])
        else:
            wait(y_in2.at[X_FIRST.index(i)], r3.at[i])
            part_of_all = gi.at[h, x, q]
            share(NX, x, "x", part_of_all, part_of_all, r4.at[i])

    def finish(i):
        wait(y_in1.at[Y_FIRST.index(i)] if i in Y_FIRST else x_in1.at[X_FIRST.index(i)], r4.at[i])

    for i in ORDER:
        stage0(i)
    z_out(0)

    loads[4].wait()
    grad[0:D, :] = jnp.dot(inp[...], pgrad[...], preferred_element_type=F32)
    to_blocks(1)
    pair_send(1)

    events = []
    for group, times, step in ((X_FIRST, X_TIMES, X_STEP), (Y_FIRST, Y_TIMES, Y_STEP)):
        for n, stage in enumerate((stage1, stage2, stage3)):
            events += [(times[n] + step * j, i, stage) for j, i in enumerate(group)]
    events.sort(key=lambda e: e[:2])
    for t, (_, i, stage) in enumerate(events):
        stage(i)
        if t == 0:
            pair_sum(1)
            z_out(1)
    for g, out in ((0, gdown_out), (1, gup_out)):
        gsum[g] = z_sum(g).reshape(ROWS, 128)[0:BLK, 0:WID]
        pltpu.make_async_copy(gsum.at[g], out, ld_sem.at[g]).start()
    for i in ORDER:
        finish(i)
    for g, out in ((0, gdown_out), (1, gup_out)):
        pltpu.make_async_copy(gsum.at[g], out, ld_sem.at[g]).wait()
    wait(sent, send_sem)


def store(gi, gup, gdown, gi_out, gup_out, gdown_out, sem):
    pairs = [
        (gi.at[h, pl.ds(0, D)], gi_out.at[:, pl.ds(h * LANES, LANES)])
        for h in range(TOK // LANES)
    ]
    pairs += [(gup, gup_out), (gdown, gdown_out)]
    copies = [pltpu.make_async_copy(a, b, sem.at[i]) for i, (a, b) in enumerate(pairs)]
    for copy in copies:
        copy.start()
    for copy in copies:
        copy.wait()


def on_device(inputs, pre_act, cotangent, w_up, w_down):
    in_hbm = pl.BlockSpec(memory_space=pltpu.HBM)
    anywhere = pl.BlockSpec(memory_space=pl.ANY)
    dma = pltpu.SemaphoreType.DMA
    operands = [
        pltpu.with_memory_space_constraint(a, pltpu.HBM)
        for a in (inputs.T, pre_act, cotangent.T, w_up, w_down.T)
    ]
    grad_input, grad_up, grad_down = pl.pallas_call(
        kernel,
        out_shape=(
            jax.ShapeDtypeStruct((TOK // LANES, NX, QUARTERS, NY, RB, LANES), BF16),
            jax.ShapeDtypeStruct((BLK, WID), F32),
            jax.ShapeDtypeStruct((BLK, WID), F32),
        ),
        in_specs=[in_hbm] * 5,
        out_specs=(anywhere,) * 3,
        scratch_shapes=[
            pltpu.VMEM((D, TOK), BF16),
            pltpu.VMEM((TOK, WID), BF16),
            pltpu.VMEM((D, TOK), BF16),
            pltpu.VMEM((BLK, WID), BF16),
            pltpu.VMEM((BLK, WID), BF16),
            pltpu.VMEM((TOK, D), BF16),
            pltpu.VMEM((ROWS, 128), F32),
            pltpu.VMEM((TOK, 128), F32),
            pltpu.VMEM((DP, 128), F32),
            pltpu.VMEM((DP, 128), F32),
            pltpu.VMEM((2, 2 * NZ, TILES, 8, 128), BF16),
            pltpu.VMEM((TOK, 128), BF16),
            pltpu.VMEM((128, TOK), BF16),
            pltpu.VMEM((TOK // LANES, NX, QUARTERS, NY, RB, LANES), BF16),
            pltpu.VMEM((len(X_FIRST), NX - 1, NY, RB, LANES), BF16),
            pltpu.VMEM((len(X_FIRST), NY, RB, LANES), BF16),
            pltpu.VMEM((len(X_FIRST), NY - 1, RB, LANES), BF16),
            pltpu.VMEM((len(Y_FIRST), NY - 1, NX, RB, LANES), BF16),
            pltpu.VMEM((len(Y_FIRST), NX, RB, LANES), BF16),
            pltpu.VMEM((len(Y_FIRST), NX - 1, RB, LANES), BF16),
            pltpu.VMEM((len(CHUNKS), RB, LANES), BF16),
            pltpu.VMEM((2, BLK, WID), F32),
            pltpu.VMEM((2, 2, NZ, TILES, 8, 128), BF16),
            pltpu.VMEM((2, NZ, TILES, 8, 128), BF16),
            pltpu.VMEM((2, NZ, TILES, 8, 128), BF16),
            pltpu.VMEM((2, NZ - 1, TILES, 8, 128), BF16),
            pltpu.VMEM((SENT, 8, 128), BF16),
            dma((5,)), dma((2, NZ)), dma((2,)), dma((2,)), dma((2,)),
            *[dma((len(CHUNKS),)) for _ in range(4)],
            pltpu.SemaphoreType.REGULAR((8,)), dma((len(CHUNKS),)), dma,
        ],
        compiler_params=pltpu.CompilerParams(
            collective_id=0, has_side_effects=True, vmem_limit_bytes=40 << 20
        ),
    )(*operands)
    grad_input, grad_up, grad_down = pl.pallas_call(
        store,
        out_shape=(
            jax.ShapeDtypeStruct((D, TOK), BF16),
            jax.ShapeDtypeStruct((BLK, WID), F32),
            jax.ShapeDtypeStruct((BLK, WID), F32),
        ),
        in_specs=[anywhere] * 3,
        out_specs=(in_hbm,) * 3,
        scratch_shapes=[dma((TOK // LANES + 2,))],
        compiler_params=pltpu.CompilerParams(vmem_limit_bytes=4 << 20),
    )(grad_input.reshape(TOK // LANES, DP, LANES), grad_up, grad_down)
    return grad_input.T, grad_up, grad_down.T


def solution(mesh):
    split = Mesh(mesh.devices.reshape(NZ, NC, NY, NX), AXES)
    fs, tp = ("z", "c"), ("y", "x")
    return jax.shard_map(
        on_device,
        mesh=split,
        in_specs=(P(fs, None), P(fs, tp), P(fs, None), P(fs, tp), P(tp, fs)),
        out_specs=(P(fs, None), P(fs, tp), P(tp, fs)),
        check_vma=False,
    )
```

```python
import functools

import jax
import jax.numpy as jnp
from jax import lax
from jax.experimental import pallas as pl
from jax.experimental.pallas import tpu as pltpu
from jax.sharding import Mesh
from jax.sharding import PartitionSpec as P

AXES = ("z", "c", "y", "x")
NZ, NC, NY, NX = 12, 2, 8, 4
MESH_IDS = pl.DeviceIdType.MESH
F32 = jnp.float32
BF16 = jnp.bfloat16
TOK, D, WID, BLK = 256, 2016, 126, 84
DP, TILES = 2048, 11
ROWS = 8 * TILES
LANES, QUARTERS, RB = 128, 4, 16
CHUNKS = [(h, q) for h in range(TOK // LANES) for q in range(QUARTERS)]
Y_FIRST = (1,)
X_FIRST = tuple(i for i in range(len(CHUNKS)) if i not in Y_FIRST)
ORDER = tuple(range(len(CHUNKS)))
PER_CHUNK = 2 * (NY - 1 + (NX - 1) * NY) * RB // 8
assert PER_CHUNK == 2 * (NX - 1 + (NY - 1) * NX) * RB // 8
SENT = 2 * TILES * (23 + NZ + NZ - 1) + len(CHUNKS) * PER_CHUNK
LAST = (len(X_FIRST) * (NX - 1) * NY + len(Y_FIRST) * (NY - 1) * NX) * RB // 8
X_TIMES = (4.3, 9.0, 13.7)
Y_TIMES = (8.5, 15.0, 18.5)
X_STEP, Y_STEP = 1.4, 3.0


def kernel(
    inputs_hbm, pre_hbm, cot_hbm, wup_hbm, wdown_hbm,
    gi, gup_out, gdown_out,
    inp, pre, cot, wup, wdn,
    cotn, scr, pact, wc, grad, wg, pgrad, pgt, part,
    x_in1, x_sum, y_in2, y_in1, y_sum, x_in2, done, gsum,
    gs, sib, cs, zr,
    sent, ld_sem, ag_recv, ag_sib, sib_recv, z_recv,
    r1, r2, r3, r4, met, own_sem, send_sem,
):
    z, c, y, x = (lax.axis_index(a) for a in AXES)

    def zpeer(d):
        return {"z": lax.rem(z + (d + NZ), NZ)}

    def ypeer(d):
        return {"y": lax.rem(y + d, NY)}

    def xpeer(d):
        return {"x": lax.rem(x + d, NX)}

    other = {"c": 1 - c}

    def send(src, dst, rsem, to):
        pltpu.make_async_remote_copy(
            src_ref=src, dst_ref=dst, send_sem=send_sem, recv_sem=rsem,
            device_id=to, device_id_type=MESH_IDS,
        ).start()

    def wait(ref, sem):
        pltpu.make_async_copy(ref, ref, sem).wait()

    barrier = pltpu.get_barrier_semaphore()
    peers = [zpeer(d) for d in (3, -3, 2, -2, 1, -1)] + [other]
    peers += [xpeer(1), xpeer(NX - 1), ypeer(1), ypeer(NY - 1)]
    for to in peers:
        pl.semaphore_signal(barrier, inc=1, device_id=to, device_id_type=MESH_IDS)

    loads = [
        pltpu.make_async_copy(a, b, ld_sem.at[i])
        for i, (a, b) in enumerate(
            ((wdown_hbm, wdn), (wup_hbm, wup), (pre_hbm, pre), (cot_hbm, cot), (inputs_hbm, inp))
        )
    ]
    for copy in loads:
        copy.start()

    mine = 2 * z + c

    def tiles(block):
        return block.reshape(TILES, 8, 128).astype(BF16)

    scr[...] = jnp.zeros_like(scr)
    loads[0].wait()
    scr[0:BLK, 0:WID] = wdn[...].astype(F32)
    wg[0, mine] = tiles(scr[...])
    loads[1].wait()
    scr[0:BLK, 0:WID] = wup[...].astype(F32)
    wg[1, mine] = tiles(scr[...])

    pl.semaphore_wait(barrier, len(peers))

    def meet(r):
        links = [(met.at[r], ypeer(1)), (met.at[3 + r], ypeer(NY - 1))]
        if r == 0:
            links += [(met.at[6], xpeer(1)), (met.at[7], xpeer(NX - 1))]
        for sem, to in links:
            pl.semaphore_signal(sem, inc=1, device_id=to, device_id_type=MESH_IDS)

    def met_all(r):
        for i in (r, 3 + r, *((6, 7) if r == 0 else ())):
            pl.semaphore_wait(met.at[i], 1)

    meet(0)

    near = jnp.where(lax.rem(z + 3, NZ) < NZ // 2, -1, 1)
    sides = (near, -near)

    def slot(d):
        return lax.rem(d + NZ, NZ)

    def block_from(d):
        return 2 * lax.rem(z - d + NZ, NZ) + c

    def ag_own(w, *steps):
        ref = wg.at[w, mine]
        for d in steps:
            send(ref, ref, ag_recv.at[w, d % NZ], zpeer(d))

    def ag_own_pair(w):
        ref = wg.at[w, mine]
        send(ref, ref, ag_sib.at[w], other)

    def ag_wait(w, d):
        wait(wg.at[w, block_from(d)], ag_recv.at[w, slot(d)])

    def ag_relay(w, side):
        ref = wg.at[w, block_from(3 * side)]

        @pl.when(c == (1 - side) // 2)
        def _():
            send(ref, ref, ag_recv.at[w, 6], zpeer(3 * side))

        ag_step(w, 3 * side, side)

        ag_step(w, 3 * side, 2 * side)

    def ag_step(w, d, step):
        ref = wg.at[w, block_from(d)]
        send(ref, ref, ag_recv.at[w, slot(d + step)], zpeer(step))

    def ag_pass(w, d):
        ref = wg.at[w, block_from(d)]
        send(ref, ref, ag_sib.at[w], other)

    def ag_last(w):
        wait(wg.at[w, pl.ds(0, NZ)], ag_sib.at[w])

    def compact(w):
        for f in range(2 * NZ):
            wc[f * BLK : f * BLK + ROWS, :] = wg[w, f].astype(F32).reshape(ROWS, 128)

    def to_blocks(g):
        for f in range(2 * NZ):
            gs[g, f % 2, f // 2] = tiles(grad[f * BLK : f * BLK + ROWS, :])

    def pair_send(g):
        send(gs.at[g, 1 - c], sib.at[g], sib_recv.at[g], other)

    def pair_sum(g):
        wait(sib.at[g], sib_recv.at[g])
        for k in range(NZ):
            cs[g, k] = (gs[g, c, k].astype(F32) + sib[g, k].astype(F32)).astype(BF16)

    def z_out(g):
        for d in (6, 5, -5, 4, -4, 3, -3, 2, -2, 1, -1):
            to = lax.rem(z + (d + NZ), NZ)
            send(cs.at[g, to], zr.at[g, d % NZ - 1], z_recv.at[g], {"z": to})

    def z_sum(g):
        wait(zr.at[g], z_recv.at[g])
        total = cs[g, z].astype(F32)
        for k in range(NZ - 1):
            total = total + zr[g, k].astype(F32)
        return total

    for w in range(2):
        ag_own(w, 3, -3)
    for w in range(2):
        ag_own_pair(w)
        ag_own(w, 1, -1)

    wc[D:DP, :] = jnp.zeros((DP - D, 128), F32)
    grad[D:DP, :] = jnp.zeros((DP - D, 128), F32)
    pact[...] = jnp.zeros_like(pact)
    loads[2].wait()
    pact[:, 0:WID] = jnp.maximum(pre[...].astype(F32), 0.0)
    positive = pact[...]
    hidden = (positive * positive).astype(BF16)
    loads[3].wait()
    cotn[...] = cot[...].T
    grad[0:D, :] = jnp.dot(cot[...], hidden, preferred_element_type=F32)
    to_blocks(0)
    pair_send(0)

    for w in range(2):
        for side in sides:
            ag_wait(w, 3 * side)
            ag_relay(w, side)
    met_all(0)
    meet(1)
    for w in range(2):
        for side in sides:
            ag_wait(w, side)
            ag_step(w, side, side)
    for w in range(2):
        for side in sides:
            ag_pass(w, 3 * side)
            ag_pass(w, side)
    for w in range(2):
        for side in sides:
            ag_wait(w, 4 * side)
    pair_sum(0)
    met_all(1)
    meet(2)

    def ag_end(w):
        for side in sides:
            ag_pass(w, 4 * side)
        for side in sides:
            ag_wait(w, 2 * side)
            ag_pass(w, 2 * side)
        ag_wait(w, 6)
        ag_pass(w, 6)
        for side in sides:
            ag_wait(w, 5 * side)
            ag_pass(w, 5 * side)

    ag_end(0)
    ag_end(1)
    ag_last(0)
    compact(0)
    hidden_grad = jnp.dot(cotn[...], wc[0:D, :].astype(BF16), preferred_element_type=F32)
    pre_grad = 2.0 * pact[...] * hidden_grad
    pgrad[...] = pre_grad.astype(BF16)
    pgt[...] = pre_grad.T.astype(BF16)
    met_all(2)
    ag_last(1)
    compact(1)

    def others(n):
        return sorted(range(1, n), key=lambda d: -min(d, n - d))

    def scatter(n, me, axis, src, dst, rsem):
        for d in others(n):
            to = lax.rem(me + d, n)
            send(src(to), dst.at[d - 1], rsem, {axis: to})

    def share(n, me, axis, src, dst, rsem):
        for d in others(n):
            send(src, dst, rsem, {axis: lax.rem(me + d, n)})

    def total(own, arrived):
        out = own.astype(F32)
        for j in range(arrived.shape[0]):
            out = out + arrived[j].astype(F32)
        return out.astype(BF16)

    def stage0(i):
        h, q = CHUNKS[i]
        for s in range(NX):
            start = (s * QUARTERS + q) * NY * RB
            rows = wc[start : start + NY * RB, :].astype(BF16)
            half = pgt[:, h * LANES : (h + 1) * LANES]
            product = jnp.dot(rows, half, preferred_element_type=F32).astype(BF16)
            part[h, s, q] = product.reshape(NY, RB, LANES)
        if i in Y_FIRST:
            dst = y_in1.at[Y_FIRST.index(i)]
            scatter(NY, y, "y", lambda to: part.at[h, :, q, to], dst, r1.at[i])
        else:
            dst = x_in1.at[X_FIRST.index(i)]
            scatter(NX, x, "x", lambda to: part.at[h, to, q], dst, r1.at[i])

    def stage1(i):
        h, q = CHUNKS[i]
        if i in Y_FIRST:
            j = Y_FIRST.index(i)
            wait(y_in1.at[j], r1.at[i])
            y_sum[j] = total(part[h, :, q, y], y_in1.at[j])
            scatter(NX, x, "x", lambda to: y_sum.at[j, to], x_in2.at[j], r2.at[i])
        else:
            j = X_FIRST.index(i)
            wait(x_in1.at[j], r1.at[i])
            x_sum[j] = total(part[h, x, q], x_in1.at[j])
            scatter(NY, y, "y", lambda to: x_sum.at[j, to], y_in2.at[j], r2.at[i])

    def stage2(i):
        h, q = CHUNKS[i]
        to = gi.at[h, x, q, y]
        if i in Y_FIRST:
            j = Y_FIRST.index(i)
            wait(x_in2.at[j], r2.at[i])
            done[i] = total(y_sum[j, x], x_in2.at[j])
            share(NX, x, "x", done.at[i], to, r3.at[i])
        else:
            j = X_FIRST.index(i)
            wait(y_in2.at[j], r2.at[i])
            done[i] = total(x_sum[j, y], y_in2.at[j])
            share(NY, y, "y", done.at[i], to, r3.at[i])
        pltpu.make_async_copy(done.at[i], to, own_sem.at[i]).start()

    def stage3(i):
        h, q = CHUNKS[i]
        pltpu.make_async_copy(done.at[i], gi.at[h, x, q, y], own_sem.at[i]).wait()
        if i in Y_FIRST:
            wait(x_in2.at[Y_FIRST.index(i)], r3.at[i])
            part_of_all = gi.at[h, :, q, y]
            share(NY, y, "y", part_of_all, part_of_all, r4)
        else:
            wait(y_in2.at[X_FIRST.index(i)], r3.at[i])
            part_of_all = gi.at[h, x, q]
            share(NX, x, "x", part_of_all, part_of_all, r4)

    for i in ORDER:
        stage0(i)
    z_out(0)

    loads[4].wait()
    grad[0:D, :] = jnp.dot(inp[...], pgrad[...], preferred_element_type=F32)
    to_blocks(1)
    pair_send(1)

    events = []
    for group, times, step in ((X_FIRST, X_TIMES, X_STEP), (Y_FIRST, Y_TIMES, Y_STEP)):
        for n, stage in enumerate((stage1, stage2, stage3)):
            events += [(times[n] + step * j, i, stage) for j, i in enumerate(group)]
    events.sort(key=lambda e: e[:2])
    for t, (_, i, stage) in enumerate(events):
        stage(i)
        if t == 0:
            pair_sum(1)
            z_out(1)
    for g, out in ((0, gdown_out), (1, gup_out)):
        gsum[g] = z_sum(g).reshape(ROWS, 128)[0:BLK, 0:WID]
        pltpu.make_async_copy(gsum.at[g], out, ld_sem.at[g]).start()
    for g, out in ((0, gdown_out), (1, gup_out)):
        pltpu.make_async_copy(gsum.at[g], out, ld_sem.at[g]).wait()
    wait(sent.at[pl.ds(0, LAST)], r4)
    wait(sent, send_sem)


def store(gi, gup, gdown, gi_out, gup_out, gdown_out, sem):
    pairs = [
        (gi.at[h, pl.ds(0, D)], gi_out.at[:, pl.ds(h * LANES, LANES)])
        for h in range(TOK // LANES)
    ]
    pairs += [(gup, gup_out), (gdown, gdown_out)]
    copies = [pltpu.make_async_copy(a, b, sem.at[i]) for i, (a, b) in enumerate(pairs)]
    for copy in copies:
        copy.start()
    for copy in copies:
        copy.wait()


def on_device(inputs, pre_act, cotangent, w_up, w_down):
    in_hbm = pl.BlockSpec(memory_space=pltpu.HBM)
    anywhere = pl.BlockSpec(memory_space=pl.ANY)
    dma = pltpu.SemaphoreType.DMA
    operands = [
        pltpu.with_memory_space_constraint(a, pltpu.HBM)
        for a in (inputs.T, pre_act, cotangent.T, w_up, w_down.T)
    ]
    grad_input, grad_up, grad_down = pl.pallas_call(
        kernel,
        out_shape=(
            jax.ShapeDtypeStruct((TOK // LANES, NX, QUARTERS, NY, RB, LANES), BF16),
            jax.ShapeDtypeStruct((BLK, WID), F32),
            jax.ShapeDtypeStruct((BLK, WID), F32),
        ),
        in_specs=[in_hbm] * 5,
        out_specs=(anywhere,) * 3,
        scratch_shapes=[
            pltpu.VMEM((D, TOK), BF16),
            pltpu.VMEM((TOK, WID), BF16),
            pltpu.VMEM((D, TOK), BF16),
            pltpu.VMEM((BLK, WID), BF16),
            pltpu.VMEM((BLK, WID), BF16),
            pltpu.VMEM((TOK, D), BF16),
            pltpu.VMEM((ROWS, 128), F32),
            pltpu.VMEM((TOK, 128), F32),
            pltpu.VMEM((DP, 128), F32),
            pltpu.VMEM((DP, 128), F32),
            pltpu.VMEM((2, 2 * NZ, TILES, 8, 128), BF16),
            pltpu.VMEM((TOK, 128), BF16),
            pltpu.VMEM((128, TOK), BF16),
            pltpu.VMEM((TOK // LANES, NX, QUARTERS, NY, RB, LANES), BF16),
            pltpu.VMEM((len(X_FIRST), NX - 1, NY, RB, LANES), BF16),
            pltpu.VMEM((len(X_FIRST), NY, RB, LANES), BF16),
            pltpu.VMEM((len(X_FIRST), NY - 1, RB, LANES), BF16),
            pltpu.VMEM((len(Y_FIRST), NY - 1, NX, RB, LANES), BF16),
            pltpu.VMEM((len(Y_FIRST), NX, RB, LANES), BF16),
            pltpu.VMEM((len(Y_FIRST), NX - 1, RB, LANES), BF16),
            pltpu.VMEM((len(CHUNKS), RB, LANES), BF16),
            pltpu.VMEM((2, BLK, WID), F32),
            pltpu.VMEM((2, 2, NZ, TILES, 8, 128), BF16),
            pltpu.VMEM((2, NZ, TILES, 8, 128), BF16),
            pltpu.VMEM((2, NZ, TILES, 8, 128), BF16),
            pltpu.VMEM((2, NZ - 1, TILES, 8, 128), BF16),
            pltpu.VMEM((SENT, 8, 128), BF16),
            dma((5,)), dma((2, NZ)), dma((2,)), dma((2,)), dma((2,)),
            *[dma((len(CHUNKS),)) for _ in range(3)], dma,
            pltpu.SemaphoreType.REGULAR((8,)), dma((len(CHUNKS),)), dma,
        ],
        compiler_params=pltpu.CompilerParams(
            collective_id=0, has_side_effects=True, vmem_limit_bytes=40 << 20
        ),
    )(*operands)
    grad_input, grad_up, grad_down = pl.pallas_call(
        store,
        out_shape=(
            jax.ShapeDtypeStruct((D, TOK), BF16),
            jax.ShapeDtypeStruct((BLK, WID), F32),
            jax.ShapeDtypeStruct((BLK, WID), F32),
        ),
        in_specs=[anywhere] * 3,
        out_specs=(in_hbm,) * 3,
        scratch_shapes=[dma((TOK // LANES + 2,))],
        compiler_params=pltpu.CompilerParams(vmem_limit_bytes=4 << 20),
    )(grad_input.reshape(TOK // LANES, DP, LANES), grad_up, grad_down)
    return grad_input.T, grad_up, grad_down.T


def solution(mesh):
    split = Mesh(mesh.devices.reshape(NZ, NC, NY, NX), AXES)
    fs, tp = ("z", "c"), ("y", "x")
    return jax.shard_map(
        on_device,
        mesh=split,
        in_specs=(P(fs, None), P(fs, tp), P(fs, None), P(fs, tp), P(tp, fs)),
        out_specs=(P(fs, None), P(fs, tp), P(tp, fs)),
        check_vma=False,
    )
```

```python
import functools

import jax
import jax.numpy as jnp
from jax import lax
from jax.experimental import pallas as pl
from jax.experimental.pallas import tpu as pltpu
from jax.sharding import Mesh
from jax.sharding import PartitionSpec as P

AXES = ("z", "c", "y", "x")
NZ, NC, NY, NX = 12, 2, 8, 4
MESH_IDS = pl.DeviceIdType.MESH
F32 = jnp.float32
BF16 = jnp.bfloat16
TOK, D, WID, BLK = 256, 2016, 126, 84
DP, TILES = 2048, 11
ROWS = 8 * TILES
LANES, QUARTERS, RB = 128, 4, 16
CHUNKS = [(h, q) for h in range(TOK // LANES) for q in range(QUARTERS)]
Y_FIRST = (1,)
X_FIRST = tuple(i for i in range(len(CHUNKS)) if i not in Y_FIRST)
ORDER = tuple(range(len(CHUNKS)))
PER_CHUNK = 2 * (NY - 1 + (NX - 1) * NY) * RB // 8
assert PER_CHUNK == 2 * (NX - 1 + (NY - 1) * NX) * RB // 8
SENT = 2 * TILES * (23 + NZ + NZ - 1) + len(CHUNKS) * PER_CHUNK
LAST = (len(X_FIRST) * (NX - 1) * NY + len(Y_FIRST) * (NY - 1) * NX) * RB // 8
X_TIMES = (4.3, 9.0, 13.7)
Y_TIMES = (8.5, 15.0, 18.5)
X_STEP, Y_STEP = 1.4, 3.0


def kernel(
    inputs_hbm, pre_hbm, cot_hbm, wup_hbm, wdown_hbm,
    gi, gup_out, gdown_out,
    inp, pre, cot, wup, wdn,
    cotn, scr, pact, wc, grad, wg, pgrad, pgt, part,
    x_in1, x_sum, y_in2, y_in1, y_sum, x_in2, done, gsum,
    gs, sib, cs, zr,
    sent, ld_sem, ag_recv, ag_sib, sib_recv, z_recv,
    r1, r2, r4, met, send_sem,
):
    z, c, y, x = (lax.axis_index(a) for a in AXES)

    def zpeer(d):
        return {"z": lax.rem(z + (d + NZ), NZ)}

    def ypeer(d):
        return {"y": lax.rem(y + d, NY)}

    def xpeer(d):
        return {"x": lax.rem(x + d, NX)}

    other = {"c": 1 - c}

    def send(src, dst, rsem, to):
        pltpu.make_async_remote_copy(
            src_ref=src, dst_ref=dst, send_sem=send_sem, recv_sem=rsem,
            device_id=to, device_id_type=MESH_IDS,
        ).start()

    def wait(ref, sem):
        pltpu.make_async_copy(ref, ref, sem).wait()

    barrier = pltpu.get_barrier_semaphore()
    peers = [zpeer(d) for d in (3, -3, 2, -2, 1, -1)] + [other]
    peers += [xpeer(1), xpeer(NX - 1), ypeer(1), ypeer(NY - 1)]
    for to in peers:
        pl.semaphore_signal(barrier, inc=1, device_id=to, device_id_type=MESH_IDS)

    loads = [
        pltpu.make_async_copy(a, b, ld_sem.at[i])
        for i, (a, b) in enumerate(
            ((wdown_hbm, wdn), (wup_hbm, wup), (pre_hbm, pre), (cot_hbm, cot), (inputs_hbm, inp))
        )
    ]
    for copy in loads:
        copy.start()

    mine = 2 * z + c

    def tiles(block):
        return block.reshape(TILES, 8, 128).astype(BF16)

    scr[...] = jnp.zeros_like(scr)
    loads[0].wait()
    scr[0:BLK, 0:WID] = wdn[...].astype(F32)
    wg[0, mine] = tiles(scr[...])
    loads[1].wait()
    scr[0:BLK, 0:WID] = wup[...].astype(F32)
    wg[1, mine] = tiles(scr[...])

    pl.semaphore_wait(barrier, len(peers))

    def meet(r):
        links = [(met.at[r], ypeer(1)), (met.at[3 + r], ypeer(NY - 1))]
        if r == 0:
            links += [(met.at[6], xpeer(1)), (met.at[7], xpeer(NX - 1))]
        for sem, to in links:
            pl.semaphore_signal(sem, inc=1, device_id=to, device_id_type=MESH_IDS)

    def met_all(r):
        for i in (r, 3 + r, *((6, 7) if r == 0 else ())):
            pl.semaphore_wait(met.at[i], 1)

    meet(0)

    near = jnp.where(lax.rem(z + 3, NZ) < NZ // 2, -1, 1)
    sides = (near, -near)

    def slot(d):
        return lax.rem(d + NZ, NZ)

    def block_from(d):
        return 2 * lax.rem(z - d + NZ, NZ) + c

    def ag_own(w, *steps):
        ref = wg.at[w, mine]
        for d in steps:
            send(ref, ref, ag_recv.at[w, d % NZ], zpeer(d))

    def ag_own_pair(w):
        ref = wg.at[w, mine]
        send(ref, ref, ag_sib.at[w], other)

    def ag_wait(w, d):
        wait(wg.at[w, block_from(d)], ag_recv.at[w, slot(d)])

    def ag_relay(w, side):
        ref = wg.at[w, block_from(3 * side)]

        @pl.when(c == (1 - side) // 2)
        def _():
            send(ref, ref, ag_recv.at[w, 6], zpeer(3 * side))

        ag_step(w, 3 * side, side)

        ag_step(w, 3 * side, 2 * side)

    def ag_step(w, d, step):
        ref = wg.at[w, block_from(d)]
        send(ref, ref, ag_recv.at[w, slot(d + step)], zpeer(step))

    def ag_pass(w, d):
        ref = wg.at[w, block_from(d)]
        send(ref, ref, ag_sib.at[w], other)

    def ag_last(w):
        wait(wg.at[w, pl.ds(0, NZ)], ag_sib.at[w])

    def compact(w):
        for f in range(2 * NZ):
            wc[f * BLK : f * BLK + ROWS, :] = wg[w, f].astype(F32).reshape(ROWS, 128)

    def to_blocks(g):
        for f in range(2 * NZ):
            gs[g, f % 2, f // 2] = tiles(grad[f * BLK : f * BLK + ROWS, :])

    def pair_send(g):
        send(gs.at[g, 1 - c], sib.at[g], sib_recv.at[g], other)

    def pair_sum(g):
        wait(sib.at[g], sib_recv.at[g])
        for k in range(NZ):
            cs[g, k] = (gs[g, c, k].astype(F32) + sib[g, k].astype(F32)).astype(BF16)

    def z_out(g):
        for d in (6, 5, -5, 4, -4, 3, -3, 2, -2, 1, -1):
            to = lax.rem(z + (d + NZ), NZ)
            send(cs.at[g, to], zr.at[g, d % NZ - 1], z_recv.at[g], {"z": to})

    def z_sum(g):
        wait(zr.at[g], z_recv.at[g])
        total = cs[g, z].astype(F32)
        for k in range(NZ - 1):
            total = total + zr[g, k].astype(F32)
        return total

    for w in range(2):
        ag_own(w, 3, -3)
    for w in range(2):
        ag_own_pair(w)
        ag_own(w, 1, -1)

    wc[D:DP, :] = jnp.zeros((DP - D, 128), F32)
    grad[D:DP, :] = jnp.zeros((DP - D, 128), F32)
    pact[...] = jnp.zeros_like(pact)
    loads[2].wait()
    pact[:, 0:WID] = jnp.maximum(pre[...].astype(F32), 0.0)
    positive = pact[...]
    hidden = (positive * positive).astype(BF16)
    loads[3].wait()
    cotn[...] = cot[...].T
    grad[0:D, :] = jnp.dot(cot[...], hidden, preferred_element_type=F32)
    to_blocks(0)
    pair_send(0)

    for w in range(2):
        for side in sides:
            ag_wait(w, 3 * side)
            ag_relay(w, side)
    met_all(0)
    meet(1)
    for w in range(2):
        for side in sides:
            ag_wait(w, side)
            ag_step(w, side, side)
    for w in range(2):
        for side in sides:
            ag_pass(w, 3 * side)
            ag_pass(w, side)
    for w in range(2):
        for side in sides:
            ag_wait(w, 4 * side)
    pair_sum(0)
    met_all(1)
    meet(2)

    def ag_end(w):
        for side in sides:
            ag_pass(w, 4 * side)
        for side in sides:
            ag_wait(w, 2 * side)
            ag_pass(w, 2 * side)
        ag_wait(w, 6)
        ag_pass(w, 6)
        for side in sides:
            ag_wait(w, 5 * side)
            ag_pass(w, 5 * side)

    ag_end(0)
    ag_end(1)
    ag_last(0)
    compact(0)
    hidden_grad = jnp.dot(cotn[...], wc[0:D, :].astype(BF16), preferred_element_type=F32)
    pre_grad = 2.0 * pact[...] * hidden_grad
    pgrad[...] = pre_grad.astype(BF16)
    pgt[...] = pre_grad.T.astype(BF16)
    met_all(2)
    ag_last(1)
    compact(1)

    def others(n):
        return sorted(range(1, n), key=lambda d: -min(d, n - d))

    def scatter(n, me, axis, src, dst, rsem):
        for d in others(n):
            to = lax.rem(me + d, n)
            send(src(to), dst.at[d - 1], rsem, {axis: to})

    def share(n, me, axis, src, dst, rsem):
        for d in others(n):
            send(src, dst, rsem, {axis: lax.rem(me + d, n)})

    def total(own, arrived):
        out = own.astype(F32)
        for j in range(arrived.shape[0]):
            out = out + arrived[j].astype(F32)
        return out.astype(BF16)

    def stage0(i):
        h, q = CHUNKS[i]
        for s in range(NX):
            start = (s * QUARTERS + q) * NY * RB
            rows = wc[start : start + NY * RB, :].astype(BF16)
            half = pgt[:, h * LANES : (h + 1) * LANES]
            product = jnp.dot(rows, half, preferred_element_type=F32).astype(BF16)
            part[h, s, q] = product.reshape(NY, RB, LANES)
        if i in Y_FIRST:
            dst = y_in1.at[Y_FIRST.index(i)]
            scatter(NY, y, "y", lambda to: part.at[h, :, q, to], dst, r1.at[i])
        else:
            dst = x_in1.at[X_FIRST.index(i)]
            scatter(NX, x, "x", lambda to: part.at[h, to, q], dst, r1.at[i])

    def stage1(i):
        h, q = CHUNKS[i]
        if i in Y_FIRST:
            j = Y_FIRST.index(i)
            wait(y_in1.at[j], r1.at[i])
            y_sum[j] = total(part[h, :, q, y], y_in1.at[j])
            scatter(NX, x, "x", lambda to: y_sum.at[j, to], x_in2.at[j], r2.at[i])
        else:
            j = X_FIRST.index(i)
            wait(x_in1.at[j], r1.at[i])
            x_sum[j] = total(part[h, x, q], x_in1.at[j])
            scatter(NY, y, "y", lambda to: x_sum.at[j, to], y_in2.at[j], r2.at[i])

    def stage2(i):
        h, q = CHUNKS[i]
        to = gi.at[h, x, q, y]
        if i in Y_FIRST:
            j = Y_FIRST.index(i)
            wait(x_in2.at[j], r2.at[i])
            done[i] = total(y_sum[j, x], x_in2.at[j])
            share(NX, x, "x", done.at[i], to, r1.at[i])
        else:
            j = X_FIRST.index(i)
            wait(y_in2.at[j], r2.at[i])
            done[i] = total(x_sum[j, y], y_in2.at[j])
            share(NY, y, "y", done.at[i], to, r1.at[i])
        pltpu.make_async_copy(done.at[i], to, r2.at[i]).start()

    def stage3(i):
        h, q = CHUNKS[i]
        pltpu.make_async_copy(done.at[i], gi.at[h, x, q, y], r2.at[i]).wait()
        if i in Y_FIRST:
            wait(x_in2.at[Y_FIRST.index(i)], r1.at[i])
            part_of_all = gi.at[h, :, q, y]
            share(NY, y, "y", part_of_all, part_of_all, r4)
        else:
            wait(y_in2.at[X_FIRST.index(i)], r1.at[i])
            part_of_all = gi.at[h, x, q]
            share(NX, x, "x", part_of_all, part_of_all, r4)

    for i in ORDER:
        stage0(i)
    z_out(0)

    loads[4].wait()
    grad[0:D, :] = jnp.dot(inp[...], pgrad[...], preferred_element_type=F32)
    to_blocks(1)
    pair_send(1)

    events = []
    for group, times, step in ((X_FIRST, X_TIMES, X_STEP), (Y_FIRST, Y_TIMES, Y_STEP)):
        for n, stage in enumerate((stage1, stage2, stage3)):
            events += [(times[n] + step * j, i, stage) for j, i in enumerate(group)]
    events.sort(key=lambda e: e[:2])
    for t, (_, i, stage) in enumerate(events):
        stage(i)
        if t == 0:
            pair_sum(1)
            z_out(1)
    for g, out in ((0, gdown_out), (1, gup_out)):
        gsum[g] = z_sum(g).reshape(ROWS, 128)[0:BLK, 0:WID]
        pltpu.make_async_copy(gsum.at[g], out, ld_sem.at[g]).start()
    for g, out in ((0, gdown_out), (1, gup_out)):
        pltpu.make_async_copy(gsum.at[g], out, ld_sem.at[g]).wait()
    wait(sent.at[pl.ds(0, LAST)], r4)
    wait(sent, send_sem)


def store(gi, gup, gdown, gi_out, gup_out, gdown_out, sem):
    pairs = [
        (gi.at[h, pl.ds(0, D)], gi_out.at[:, pl.ds(h * LANES, LANES)])
        for h in range(TOK // LANES)
    ]
    pairs += [(gup, gup_out), (gdown, gdown_out)]
    copies = [pltpu.make_async_copy(a, b, sem.at[i]) for i, (a, b) in enumerate(pairs)]
    for copy in copies:
        copy.start()
    for copy in copies:
        copy.wait()


def on_device(inputs, pre_act, cotangent, w_up, w_down):
    in_hbm = pl.BlockSpec(memory_space=pltpu.HBM)
    anywhere = pl.BlockSpec(memory_space=pl.ANY)
    dma = pltpu.SemaphoreType.DMA
    operands = [
        pltpu.with_memory_space_constraint(a, pltpu.HBM)
        for a in (inputs.T, pre_act, cotangent.T, w_up, w_down.T)
    ]
    grad_input, grad_up, grad_down = pl.pallas_call(
        kernel,
        out_shape=(
            jax.ShapeDtypeStruct((TOK // LANES, NX, QUARTERS, NY, RB, LANES), BF16),
            jax.ShapeDtypeStruct((BLK, WID), F32),
            jax.ShapeDtypeStruct((BLK, WID), F32),
        ),
        in_specs=[in_hbm] * 5,
        out_specs=(anywhere,) * 3,
        scratch_shapes=[
            pltpu.VMEM((D, TOK), BF16),
            pltpu.VMEM((TOK, WID), BF16),
            pltpu.VMEM((D, TOK), BF16),
            pltpu.VMEM((BLK, WID), BF16),
            pltpu.VMEM((BLK, WID), BF16),
            pltpu.VMEM((TOK, D), BF16),
            pltpu.VMEM((ROWS, 128), F32),
            pltpu.VMEM((TOK, 128), F32),
            pltpu.VMEM((DP, 128), F32),
            pltpu.VMEM((DP, 128), F32),
            pltpu.VMEM((2, 2 * NZ, TILES, 8, 128), BF16),
            pltpu.VMEM((TOK, 128), BF16),
            pltpu.VMEM((128, TOK), BF16),
            pltpu.VMEM((TOK // LANES, NX, QUARTERS, NY, RB, LANES), BF16),
            pltpu.VMEM((len(X_FIRST), NX - 1, NY, RB, LANES), BF16),
            pltpu.VMEM((len(X_FIRST), NY, RB, LANES), BF16),
            pltpu.VMEM((len(X_FIRST), NY - 1, RB, LANES), BF16),
            pltpu.VMEM((len(Y_FIRST), NY - 1, NX, RB, LANES), BF16),
            pltpu.VMEM((len(Y_FIRST), NX, RB, LANES), BF16),
            pltpu.VMEM((len(Y_FIRST), NX - 1, RB, LANES), BF16),
            pltpu.VMEM((len(CHUNKS), RB, LANES), BF16),
            pltpu.VMEM((2, BLK, WID), F32),
            pltpu.VMEM((2, 2, NZ, TILES, 8, 128), BF16),
            pltpu.VMEM((2, NZ, TILES, 8, 128), BF16),
            pltpu.VMEM((2, NZ, TILES, 8, 128), BF16),
            pltpu.VMEM((2, NZ - 1, TILES, 8, 128), BF16),
            pltpu.VMEM((SENT, 8, 128), BF16),
            dma((5,)), dma((2, NZ)), dma((2,)), dma((2,)), dma((2,)),
            *[dma((len(CHUNKS),)) for _ in range(2)], dma,
            pltpu.SemaphoreType.REGULAR((8,)), dma,
        ],
        compiler_params=pltpu.CompilerParams(
            collective_id=0, has_side_effects=True, vmem_limit_bytes=40 << 20
        ),
    )(*operands)
    grad_input, grad_up, grad_down = pl.pallas_call(
        store,
        out_shape=(
            jax.ShapeDtypeStruct((D, TOK), BF16),
            jax.ShapeDtypeStruct((BLK, WID), F32),
            jax.ShapeDtypeStruct((BLK, WID), F32),
        ),
        in_specs=[anywhere] * 3,
        out_specs=(in_hbm,) * 3,
        scratch_shapes=[dma((TOK // LANES + 2,))],
        compiler_params=pltpu.CompilerParams(vmem_limit_bytes=4 << 20),
    )(grad_input.reshape(TOK // LANES, DP, LANES), grad_up, grad_down)
    return grad_input.T, grad_up, grad_down.T


def solution(mesh):
    split = Mesh(mesh.devices.reshape(NZ, NC, NY, NX), AXES)
    fs, tp = ("z", "c"), ("y", "x")
    return jax.shard_map(
        on_device,
        mesh=split,
        in_specs=(P(fs, None), P(fs, tp), P(fs, None), P(fs, tp), P(tp, fs)),
        out_specs=(P(fs, None), P(fs, tp), P(tp, fs)),
        check_vma=False,
    )
```
